32 devices in a mesh: sp: 8 (over z, x), tp: 4 (over y, core).
Axes of the slice: x: 2, y: 2, z: 4, core: 2. Of those that a mesh axis runs over, the one named last changes fastest.
Arguments:
- tokens: bfloat16 [1024, 1024], P(('sp', 'tp')), may hold values from -13 to 13, as said below
- norm_gain: float32 [1024], replicated, may hold values from 0.5 to 1.5
- query_weight: bfloat16 [1024, 4096], P(None, 'tp'), may hold values from -0.1875 to 0.1875
- key_weight: bfloat16 [1024, 512], P(None, 'tp'), may hold values from -0.1875 to 0.1875
- value_weight: bfloat16 [1024, 512], P(None, 'tp'), may hold values from -0.1875 to 0.1875
- query_gain: float32 [128], replicated, may hold values from 0.5 to 1.5
- key_gain: float32 [128], replicated, may hold values from 0.5 to 1.5
- output_weight: bfloat16 [4096, 1024], P('tp'), may hold values from -0.25 to 0.25
Outputs:
- mixed: bfloat16 [1024, 1024], P(('sp', 'tp'))
The draws below stay inside these ranges and needn't reach their ends.
Inputs may be any that keep to these rules, and one draw needn't show every extreme that they name: Every entry of tokens lies between -13 and 13.
All inputs are finite; a program needn't handle non-finite values.
Results may differ from the reference program's by a relative error of at most 0.015.
Values may be sent and summed in bfloat16 or wider, within the bound.
A program may use at most 64 MiB of HBM per device.

```python
import jax
import jax.numpy as jnp
from jax import lax

D = 1024
HEADS = 32
KV_HEADS = 4
HEAD_DIM = 128
GRID_W = 64
TOK_SP = 128
TOKENS = 1024


def draw_tokens(key, part):
    noise_key = jax.random.fold_in(key, 11)
    region_key = jax.random.fold_in(key, 12)
    regions = TOKENS // TOK_SP
    noise_part = jnp.clip(jax.random.normal(noise_key, (TOKENS, D), jnp.float32), -4.0, 4.0)
    centres = 1.5 * jnp.clip(jax.random.normal(region_key, (regions, D), jnp.float32), -3.0, 3.0)
    spread_means = jnp.broadcast_to(centres[:, None, :], (regions, TOK_SP, D)).reshape(TOKENS, D)
    return (noise_part + spread_means).astype(jnp.bfloat16)


def shard_levels(stream_key, extent, cuts, smallest, largest):
    level = 1.0
    for dim, blocks in cuts:
        steps = jax.random.uniform(jax.random.fold_in(jax.random.fold_in(stream_key, 6), dim), (blocks,), jnp.float32, smallest / len(cuts), largest / len(cuts))
        level = level * jnp.repeat(jnp.exp(steps), extent[dim] // blocks).reshape((-1,) + (1,) * (len(extent) - 1 - dim))
    return level


def centred(key, extent, deviation, limit, shards=(), held_as=jnp.bfloat16):
    array = deviation * jax.random.normal(key, extent, jnp.float32)
    if shards:
        array = array * shard_levels(key, extent, shards, -0.22, 0.18)
    return jnp.clip(array, -limit, limit).astype(held_as)


def setup_inputs(seed: int = 0) -> dict:
    key_list = jax.random.split(jax.random.key(seed), 9)
    tokens = draw_tokens(jax.random.fold_in(key_list[8], 71), 0)
    norm_gain = jnp.clip(1.0 + 0.1 * jax.random.normal(key_list[1], (D,), jnp.float32), 0.5, 1.5)
    query_weight = centred(key_list[2], (D, HEADS * HEAD_DIM), D ** -0.5, 0.1875, ((1, 4),))
    key_weight = centred(key_list[3], (D, KV_HEADS * HEAD_DIM), D ** -0.5, 0.1875, ((1, 4),))
    value_weight = centred(key_list[4], (D, KV_HEADS * HEAD_DIM), D ** -0.5, 0.1875, ((1, 4),))
    query_gain = jnp.clip(1.0 + 0.1 * jax.random.normal(key_list[5], (HEAD_DIM,), jnp.float32), 0.5, 1.5)
    key_gain = jnp.clip(1.0 + 0.1 * jax.random.normal(key_list[6], (HEAD_DIM,), jnp.float32), 0.5, 1.5)
    output_weight = centred(key_list[7], (HEADS * HEAD_DIM, D), (HEADS * HEAD_DIM * TOK_SP // TOKENS) ** -0.5, 0.25, ((0, 4),))
    return dict(tokens=tokens, norm_gain=norm_gain, query_weight=query_weight, key_weight=key_weight, value_weight=value_weight, query_gain=query_gain, key_gain=key_gain, output_weight=output_weight)


epsilon = 1e-06
rotary_base = 10000.0

def rotation_tables(first_position, length, head_dim):
    positions = first_position + lax.iota(jnp.int32, length)
    grid_row = (positions // GRID_W).astype(jnp.float32)
    grid_column = (positions % GRID_W).astype(jnp.float32)
    axis_dim = head_dim // 2
    frequencies = rotary_base ** (-jnp.arange(0, axis_dim, 2, dtype=jnp.float32) / axis_dim)
    angles = jnp.concatenate([grid_row[:, None] * frequencies[None, :], grid_column[:, None] * frequencies[None, :]], axis=-1)
    return (jnp.cos(angles), jnp.sin(angles))

def normalize_rotate(projected, gain, cosine, sine):
    widened = projected.astype(jnp.float32)
    scaled = widened * lax.rsqrt(lax.optimization_barrier(jnp.mean(widened * widened, axis=-1, keepdims=True)) + epsilon) * gain.astype(jnp.float32)
    paired = scaled.reshape(scaled.shape[:-1] + (scaled.shape[-1] // 2, 2))
    even_half = paired[..., 0]
    odd_half = paired[..., 1]
    cosine_rows = cosine[:, None, :]
    sine_rows = sine[:, None, :]
    turned = jnp.stack([even_half * cosine_rows - odd_half * sine_rows, even_half * sine_rows + odd_half * cosine_rows], axis=-1)
    return turned.reshape(projected.shape).astype(jnp.bfloat16)

def rms_rows(tokens, norm_gain):
    widened = tokens.astype(jnp.float32)
    scaled = widened * lax.rsqrt(lax.optimization_barrier(jnp.mean(widened * widened, axis=-1, keepdims=True)) + epsilon)
    return (scaled * norm_gain.astype(jnp.float32)).astype(jnp.bfloat16)

def reference(tokens, norm_gain, query_weight, key_weight, value_weight, query_gain, key_gain, output_weight):
    normed = rms_rows(tokens, norm_gain)
    query_part = jnp.dot(normed, query_weight, preferred_element_type=jnp.float32).astype(jnp.bfloat16)
    key_part = jnp.dot(normed, key_weight, preferred_element_type=jnp.float32).astype(jnp.bfloat16)
    value_part = jnp.dot(normed, value_weight, preferred_element_type=jnp.float32).astype(jnp.bfloat16)
    cosine, sine = rotation_tables(0, TOKENS, HEAD_DIM)
    queries = normalize_rotate(query_part.reshape(TOKENS, HEADS, HEAD_DIM), query_gain, cosine, sine)
    keys = normalize_rotate(key_part.reshape(TOKENS, KV_HEADS, HEAD_DIM), key_gain, cosine, sine)
    key_all = keys.astype(jnp.float32)
    value_all = value_part.reshape(TOKENS, KV_HEADS, HEAD_DIM).astype(jnp.float32)
    group_size = HEADS // KV_HEADS
    block_count = TOKENS // GRID_W
    query_blocks = queries.reshape(block_count, GRID_W, KV_HEADS, group_size, HEAD_DIM)
    scale = HEAD_DIM ** (-0.5)

    def one_block(query_block):
        scores = jnp.einsum('qkgd,skd->kgqs', query_block.astype(jnp.float32), key_all, precision=lax.Precision.HIGHEST) * scale
        highest = lax.optimization_barrier(jnp.max(scores, axis=-1, keepdims=True))
        weights = jnp.exp(scores - highest)
        denominator = lax.optimization_barrier(jnp.sum(weights, axis=-1))
        rounded = lax.optimization_barrier(weights.astype(jnp.bfloat16)).astype(jnp.float32)
        numerator = jnp.einsum('kgqs,skd->kgqd', rounded, value_all, precision=lax.Precision.HIGHEST)
        return (numerator / denominator[..., None]).astype(jnp.bfloat16)
    attended = lax.map(one_block, query_blocks)
    attended = attended.transpose(0, 3, 1, 2, 4).reshape(TOKENS, HEADS * HEAD_DIM)
    return jnp.dot(attended, output_weight, preferred_element_type=jnp.float32).astype(jnp.bfloat16)
```

```python
import functools
import math

import jax
import jax.numpy as jnp
import numpy as np
from jax import lax
from jax.experimental import pallas as pl
from jax.experimental.pallas import tpu as pltpu

from jax.sharding import PartitionSpec as P

GRID_W = 64
EPS = 1e-06
ROTARY_BASE = 10000.0
MESH = pl.DeviceIdType.MESH
F32 = jnp.float32
BF16 = jnp.bfloat16
UNROLL = 8


def angle_tables(grid_rows, head_dim):
    half = head_dim // 2
    freq = np.float32(ROTARY_BASE) ** (-np.arange(0, half, 2, dtype=np.float32) / np.float32(half))
    freq = np.repeat(freq.astype(np.float32), 2)
    sign = np.tile(np.array([-1.0, 1.0], np.float32), half // 2)
    zero = lambda n: np.zeros((n, half), np.float32)
    row = np.arange(grid_rows, dtype=np.float32)[:, None] * freq[None, :]
    col = np.arange(GRID_W, dtype=np.float32)[:, None] * freq[None, :]
    rows = np.stack(
        [
            np.concatenate([np.cos(row), zero(grid_rows)], 1),
            np.concatenate([np.sin(row) * sign, zero(grid_rows)], 1),
        ]
    )
    cols = np.stack(
        [
            np.concatenate([zero(GRID_W), np.cos(col)], 1),
            np.concatenate([zero(GRID_W), np.sin(col) * sign], 1),
        ]
    )
    return rows.astype(np.float32), cols.astype(np.float32)


def repeat(start, stop, body):
    if stop - start <= UNROLL:
        for i in range(start, stop):
            body(i)
    else:
        lax.fori_loop(start, stop, lambda i, c: (body(i), c)[1], 0)


class PairExchange:
    def __init__(self, axis, n, buf, send, recv):
        self.axis, self.n, self.buf, self.send, self.recv = axis, n, buf, send, recv
        self.half = n // 2
        self.me = lax.axis_index(axis)
        self.partner = self.me + 1 - 2 * (self.me % 2)

    def hop(self, i):
        if isinstance(i, int):
            return (i + 1) // 2 if i % 2 == 1 else self.half - i // 2
        return (i % 2) * ((i + 1) // 2) + (1 - i % 2) * (self.half - i // 2)

    def source(self, i):
        return lax.rem(self.me + self.n - 2 * self.hop(i), self.n)

    def pair_of(self, slot):
        return slot + 1 - 2 * (slot % 2)

    def copy(self, slot, sem, target):
        return pltpu.make_async_remote_copy(
            src_ref=self.buf.at[slot],
            dst_ref=self.buf.at[slot],
            send_sem=self.send.at[sem],
            recv_sem=self.recv.at[slot],
            device_id={self.axis: target},
            device_id_type=MESH,
        )

    def greet(self, barrier):
        pl.semaphore_signal(barrier, inc=1, device_id={self.axis: self.partner}, device_id_type=MESH)

        def one(i):
            target = lax.rem(self.me + 2 * i, self.n)
            pl.semaphore_signal(barrier, inc=1, device_id={self.axis: target}, device_id_type=MESH)

        repeat(1, self.half, one)
        return self.half

    def start(self):
        def one(i):
            self.copy(self.me, i, lax.rem(self.me + 2 * self.hop(i), self.n)).start()

        self.copy(self.me, 0, self.partner).start()
        repeat(1, self.half, one)

    def forward(self, i):
        slot = self.source(i)
        self.copy(slot, 0, self.partner).wait_recv()
        self.copy(slot, self.half + i, self.partner).start()

    def wait_slot(self, slot):
        self.copy(slot, 0, self.partner).wait_recv()

    def finish(self):
        def one(i):
            self.copy(self.me, i, self.partner).wait_send()

        def two(i):
            self.copy(self.me, self.half + i, self.partner).wait_send()

        repeat(0, self.half, one)
        repeat(1, self.half, two)


def layer_kernel(
    n_sp,
    n_tp,
    tokens,
    norm_gain,
    wq_hbm,
    wk_hbm,
    wv_hbm,
    query_gain,
    key_gain,
    wo_hbm,
    row_hbm,
    col_hbm,
    out,
    tok,
    gain,
    qgain,
    kgain,
    wq,
    wkv,
    wo,
    rowtab,
    coltab,
    normed,
    kv,
    q,
    num,
    den,
    att,
    own,
    part,
    got,
    lsem,
    tok_send,
    tok_recv,
    kv_send,
    kv_recv,
    rs_send,
    rs_recv,
):
    tp = lax.axis_index("tp")
    sp = lax.axis_index("sp")
    rows, width = tok.shape[1], tok.shape[2]
    block = n_tp * rows
    hd = q.shape[1]
    heads = wq.shape[1] // hd
    tokx = PairExchange("tp", n_tp, tok, tok_send, tok_recv)
    kvx = PairExchange("sp", n_sp, kv, kv_send, kv_recv)

    local = [
        (tokens, tok.at[tp]),
        (norm_gain, gain),
        (wk_hbm, wkv.at[:, pl.ds(0, hd)]),
        (wv_hbm, wkv.at[:, pl.ds(hd, hd)]),
        (key_gain, kgain),
        (query_gain, qgain),
        (row_hbm, rowtab),
        (col_hbm, coltab),
        (wq_hbm, wq),
        (wo_hbm, wo),
    ]
    copies = [pltpu.make_async_copy(a, b, lsem.at[i]) for i, (a, b) in enumerate(local)]
    barrier = pltpu.get_barrier_semaphore()
    copies[0].start()
    count = kvx.greet(barrier) + n_tp - 1
    for k in range(1, n_tp):
        target = lax.rem(tp + k, n_tp)
        pl.semaphore_signal(barrier, inc=1, device_id={"tp": target}, device_id_type=MESH)
    for c in copies[1:]:
        c.start()
    copies[0].wait()
    pl.semaphore_wait(barrier, count)

    tokx.start()

    for c in copies[1:8]:
        c.wait()
    grid_rows = block // GRID_W
    cosine, sine = [], []
    for g in range(grid_rows):
        r = sp * grid_rows + g
        cosine.append(coltab[0] + rowtab[0, pl.ds(r, 1), :])
        sine.append(coltab[1] + rowtab[1, pl.ds(r, 1), :])
    cosine = jnp.concatenate(cosine, 0)
    sine = jnp.concatenate(sine, 0)
    even = lax.broadcasted_iota(jnp.int32, (block, hd), 1) % 2 == 0

    def rotate(projected, head_gain):
        x = projected.astype(BF16).astype(F32)
        x = x * lax.rsqrt(jnp.mean(x * x, axis=-1, keepdims=True) + EPS) * head_gain
        swapped = jnp.where(even, pltpu.roll(x, hd - 1, 1), pltpu.roll(x, 1, 1))
        return (x * cosine + swapped * sine).astype(BF16)

    def norm(slot):
        x = tok[slot].astype(F32)
        x = x * lax.rsqrt(jnp.mean(x * x, axis=-1, keepdims=True) + EPS) * gain[...]
        start = pl.multiple_of(slot * rows, rows)
        normed[pl.ds(start, rows), :] = x.astype(BF16)

    norm(tp)
    for i in range(1, tokx.half):
        tokx.forward(i)
    for i in range(1, tokx.half):
        norm(tokx.source(i))
    tokx.wait_slot(tokx.partner)
    norm(tokx.partner)
    for i in range(1, tokx.half):
        slot = tokx.pair_of(tokx.source(i))
        tokx.wait_slot(slot)
        norm(slot)

    kvp = jnp.dot(normed[...], wkv[...], preferred_element_type=F32)
    kv[sp, 1] = kvp[:, hd:].astype(BF16)
    kv[sp, 0] = rotate(kvp[:, :hd], kgain[...])
    kvx.start()

    copies[8].wait()
    step = 2 * hd
    for c in range(wq.shape[1] // step):
        qp = jnp.dot(normed[...], wq[:, c * step : (c + 1) * step], preferred_element_type=F32)
        for h in range(2):
            base = (2 * c + h) * block
            q[base : base + block, :] = rotate(qp[:, h * hd : (h + 1) * hd], qgain[...])

    factor = hd**-0.5 * math.log2(math.e)

    def fold(slot, first):
        low = slot - slot % 2
        keys = kv[pl.ds(low, 2), 0].reshape(2 * block, hd)
        values = kv[pl.ds(low, 2), 1].reshape(2 * block, hd)
        for h in range(heads):
            span = slice(h * block, (h + 1) * block)
            s = lax.dot_general(
                q[span, :], keys, (((1,), (1,)), ((), ())), preferred_element_type=F32
            )
            w = jnp.exp2(s * factor)
            d = w[:, :hd]
            for j in range(1, 2 * block // hd):
                d = d + w[:, j * hd : (j + 1) * hd]
            v = jnp.dot(w.astype(BF16), values, preferred_element_type=F32)
            if first:
                den[span, :] = d
                num[span, :] = v
            else:
                den[span, :] += d
                num[span, :] += v

    kvx.forward(1)
    kvx.wait_slot(kvx.partner)
    fold(sp, True)

    def middle(i):
        kvx.forward(i)
        slot = kvx.source(i - 1)
        kvx.wait_slot(kvx.pair_of(slot))
        fold(slot, False)

    repeat(2, kvx.half, middle)
    slot = kvx.source(kvx.half - 1)
    kvx.wait_slot(kvx.pair_of(slot))
    fold(slot, False)

    for h in range(heads):
        span = slice(h * block, (h + 1) * block)
        total = jnp.sum(den[span, :], axis=-1, keepdims=True)
        att[:, h * hd : (h + 1) * hd] = (num[span, :] / total).astype(BF16)

    copies[9].wait()
    chunks, chunk = part.shape[0], part.shape[3]

    def share(c, k):
        target = lax.rem(tp + k, n_tp)
        return pltpu.make_async_remote_copy(
            src_ref=part.at[c, target],
            dst_ref=got.at[c, k - 1],
            send_sem=rs_send.at[c, k - 1],
            recv_sem=rs_recv.at[c, k - 1],
            device_id={"tp": target},
            device_id_type=MESH,
        )

    order = [n_tp // 2] + [k for k in range(1, n_tp) if k != n_tp // 2]
    for c in range(chunks):
        p = jnp.dot(att[...], wo[:, c * chunk : (c + 1) * chunk], preferred_element_type=F32)
        own[c] = p.reshape(n_tp, rows, chunk)
        part[c] = p.astype(BF16).reshape(n_tp, rows, chunk)
        for k in order:
            share(c, k).start()
    for c in range(chunks):
        total = own[c, tp]
        for k in order:
            share(c, k).wait_recv()
            total = total + got[c, k - 1].astype(F32)
        out[:, c * chunk : (c + 1) * chunk] = total.astype(BF16)

    for c in range(chunks):
        for k in order:
            share(c, k).wait_send()
    tokx.finish()
    kvx.finish()


def solution(mesh):
    n_sp, n_tp = mesh.shape["sp"], mesh.shape["tp"]

    def per_device(tokens, norm_gain, wq, wk, wv, query_gain, key_gain, wo):
        rows, width = tokens.shape
        hd = query_gain.shape[0]
        block = rows * n_tp
        heads = wq.shape[1] // hd
        out_width = wo.shape[1]
        chunks = 4
        chunk = out_width // chunks
        row_np, col_np = angle_tables(block * n_sp // GRID_W, hd)
        vmem = pltpu.VMEM
        dma = pltpu.SemaphoreType.DMA
        any_spec = pl.BlockSpec(memory_space=pl.ANY)
        return pl.pallas_call(
            functools.partial(layer_kernel, n_sp, n_tp),
            out_shape=jax.ShapeDtypeStruct((rows, out_width), BF16),
            in_specs=[any_spec] * 10,
            out_specs=pl.BlockSpec(memory_space=pltpu.VMEM),
            scratch_shapes=[
                vmem((n_tp, rows, width), BF16),
                vmem((1, width), F32),
                vmem((1, hd), F32),
                vmem((1, hd), F32),
                vmem(wq.shape, BF16),
                vmem((width, 2 * hd), BF16),
                vmem(wo.shape, BF16),
                vmem(row_np.shape, F32),
                vmem(col_np.shape, F32),
                vmem((block, width), BF16),
                vmem((n_sp, 2, block, hd), BF16),
                vmem((heads * block, hd), BF16),
                vmem((heads * block, hd), F32),
                vmem((heads * block, hd), F32),
                vmem((block, heads * hd), BF16),
                vmem((chunks, n_tp, rows, chunk), F32),
                vmem((chunks, n_tp, rows, chunk), BF16),
                vmem((chunks, n_tp - 1, rows, chunk), BF16),
                dma((10,)),
                dma((n_tp,)),
                dma((n_tp,)),
                dma((n_sp,)),
                dma((n_sp,)),
                dma((chunks, n_tp - 1)),
                dma((chunks, n_tp - 1)),
            ],
            compiler_params=pltpu.CompilerParams(
                collective_id=0, has_side_effects=True, vmem_limit_bytes=60 * 1024 * 1024
            ),
        )(
            tokens,
            norm_gain.reshape(1, width),
            wq,
            wk,
            wv,
            query_gain.reshape(1, hd),
            key_gain.reshape(1, hd),
            wo,
            jnp.asarray(row_np),
            jnp.asarray(col_np),
        )

    return jax.shard_map(
        per_device,
        mesh=mesh,
        in_specs=(
            P(("sp", "tp"), None),
            P(),
            P(None, "tp"),
            P(None, "tp"),
            P(None, "tp"),
            P(),
            P(),
            P("tp", None),
        ),
        out_specs=P(("sp", "tp"), None),
        check_vma=False,
    )
```

```python
import functools
import math

import jax
import jax.numpy as jnp
import numpy as np
from jax import lax
from jax.experimental import pallas as pl
from jax.experimental.pallas import tpu as pltpu

from jax.sharding import PartitionSpec as P

GRID_W = 64
EPS = 1e-06
ROTARY_BASE = 10000.0
MESH = pl.DeviceIdType.MESH
F32 = jnp.float32
BF16 = jnp.bfloat16
UNROLL = 8


def angle_tables(grid_rows, head_dim):
    half = head_dim // 2
    freq = np.float32(ROTARY_BASE) ** (-np.arange(0, half, 2, dtype=np.float32) / np.float32(half))
    freq = np.repeat(freq.astype(np.float32), 2)
    sign = np.tile(np.array([-1.0, 1.0], np.float32), half // 2)
    zero = lambda n: np.zeros((n, half), np.float32)
    row = np.arange(grid_rows, dtype=np.float32)[:, None] * freq[None, :]
    col = np.arange(GRID_W, dtype=np.float32)[:, None] * freq[None, :]
    rows = np.stack(
        [
            np.concatenate([np.cos(row), zero(grid_rows)], 1),
            np.concatenate([np.sin(row) * sign, zero(grid_rows)], 1),
        ]
    )
    cols = np.stack(
        [
            np.concatenate([zero(GRID_W), np.cos(col)], 1),
            np.concatenate([zero(GRID_W), np.sin(col) * sign], 1),
        ]
    )
    return rows.astype(np.float32), cols.astype(np.float32)


def repeat(start, stop, body):
    if stop - start <= UNROLL:
        for i in range(start, stop):
            body(i)
    else:
        lax.fori_loop(start, stop, lambda i, c: (body(i), c)[1], 0)


class GroupExchange:
    def __init__(self, axis, n, size, buf, send, recv):
        self.axis, self.size, self.buf, self.send, self.recv = axis, size, buf, send, recv
        self.groups = n // size
        self.me = lax.axis_index(axis)
        self.group, self.place = self.me // size, self.me % size
        self.parts = buf.shape[0]

    def mate(self, j):
        return self.group * self.size + lax.rem(self.place + j, self.size)

    def peer(self, i):
        return lax.rem(self.group + i, self.groups) * self.size + self.place

    def source(self, i, j=0):
        group = lax.rem(self.group + self.groups - i, self.groups)
        return group * self.size + lax.rem(self.place + j, self.size)

    def copy(self, part, slot, sem, target):
        return pltpu.make_async_remote_copy(
            src_ref=self.buf.at[part, slot],
            dst_ref=self.buf.at[part, slot],
            send_sem=self.send.at[part, sem],
            recv_sem=self.recv.at[part, slot],
            device_id={self.axis: target},
            device_id_type=MESH,
        )

    def greet(self, barrier):
        def one(target):
            pl.semaphore_signal(barrier, inc=1, device_id={self.axis: target}, device_id_type=MESH)

        repeat(1, self.groups, lambda i: one(self.peer(i)))
        for j in range(1, self.size):
            one(self.mate(j))
        return self.groups + self.size - 2

    def start(self):
        def one(i):
            for part in range(self.parts):
                self.copy(part, self.me, self.size - 2 + i, self.peer(i)).start()

        repeat(1, self.groups, one)
        for j in range(1, self.size):
            for part in range(self.parts):
                self.copy(part, self.me, j - 1, self.mate(j)).start()

    def forward(self, i):
        slot = self.source(i)
        first = self.groups + self.size - 2 + (i - 1) * (self.size - 1)
        for part in range(self.parts):
            self.copy(part, slot, 0, self.peer(i)).wait_recv()
            for j in range(1, self.size):
                self.copy(part, slot, first + j - 1, self.mate(j)).start()

    def wait_slot(self, slot):
        for part in range(self.parts):
            self.copy(part, slot, 0, self.mate(1)).wait_recv()

    def finish(self):
        def one(i):
            for part in range(self.parts):
                self.copy(part, self.me, i, self.mate(1)).wait_send()

        repeat(0, self.groups * self.size - 1, one)


def layer_kernel(
    n_sp,
    n_tp,
    tokens,
    norm_gain,
    wq_hbm,
    wk_hbm,
    wv_hbm,
    query_gain,
    key_gain,
    wo_hbm,
    row_hbm,
    col_hbm,
    out,
    tok,
    gain,
    qgain,
    kgain,
    wq,
    wkv,
    wo,
    rowtab,
    coltab,
    normed,
    kv,
    q,
    num,
    den,
    att,
    own,
    part,
    got,
    lsem,
    tok_send,
    tok_recv,
    kv_send,
    kv_recv,
    rs_send,
    rs_recv,
):
    tp = lax.axis_index("tp")
    sp = lax.axis_index("sp")
    rows, width = tok.shape[2], tok.shape[3]
    block = n_tp * rows
    hd = q.shape[1]
    heads = wq.shape[1] // hd
    tokx = GroupExchange("tp", n_tp, 2, tok, tok_send, tok_recv)
    kvx = GroupExchange("sp", n_sp, 4, kv, kv_send, kv_recv)

    local = [
        (tokens, tok.at[0, tp]),
        (norm_gain, gain),
        (wk_hbm, wkv.at[:, pl.ds(0, hd)]),
        (wv_hbm, wkv.at[:, pl.ds(hd, hd)]),
        (key_gain, kgain),
        (query_gain, qgain),
        (row_hbm, rowtab),
        (col_hbm, coltab),
        (wq_hbm, wq),
        (wo_hbm, wo),
    ]
    copies = [pltpu.make_async_copy(a, b, lsem.at[i]) for i, (a, b) in enumerate(local)]
    barrier = pltpu.get_barrier_semaphore()
    copies[0].start()
    count = kvx.greet(barrier) + n_tp - 1
    for k in range(1, n_tp):
        target = lax.rem(tp + k, n_tp)
        pl.semaphore_signal(barrier, inc=1, device_id={"tp": target}, device_id_type=MESH)
    for c in copies[1:]:
        c.start()
    copies[0].wait()
    pl.semaphore_wait(barrier, count)

    tokx.start()

    for c in copies[1:8]:
        c.wait()
    grid_rows = block // GRID_W
    cosine, sine = [], []
    for g in range(grid_rows):
        r = sp * grid_rows + g
        cosine.append(coltab[0] + rowtab[0, pl.ds(r, 1), :])
        sine.append(coltab[1] + rowtab[1, pl.ds(r, 1), :])
    cosine = jnp.concatenate(cosine, 0)
    sine = jnp.concatenate(sine, 0)
    even = lax.broadcasted_iota(jnp.int32, (block, hd), 1) % 2 == 0

    def rotate(projected, head_gain):
        x = projected.astype(BF16).astype(F32)
        x = x * lax.rsqrt(jnp.mean(x * x, axis=-1, keepdims=True) + EPS) * head_gain
        swapped = jnp.where(even, pltpu.roll(x, hd - 1, 1), pltpu.roll(x, 1, 1))
        return (x * cosine + swapped * sine).astype(BF16)

    def norm(slot):
        x = tok[0, slot].astype(F32)
        x = x * lax.rsqrt(jnp.mean(x * x, axis=-1, keepdims=True) + EPS) * gain[...]
        start = pl.multiple_of(slot * rows, rows)
        normed[pl.ds(start, rows), :] = x.astype(BF16)

    norm(tp)
    for i in range(1, tokx.groups):
        tokx.forward(i)
        norm(tokx.source(i))
    for j in range(1, tokx.size):
        tokx.wait_slot(tokx.mate(j))
        norm(tokx.mate(j))
    for i in range(1, tokx.groups):
        for j in range(1, tokx.size):
            tokx.wait_slot(tokx.source(i, j))
            norm(tokx.source(i, j))

    kvp = jnp.dot(normed[...], wkv[...], preferred_element_type=F32)
    kv[1, sp] = kvp[:, hd:].astype(BF16)
    kv[0, sp] = rotate(kvp[:, :hd], kgain[...])
    kvx.start()

    copies[8].wait()
    step = 2 * hd
    for c in range(wq.shape[1] // step):
        qp = jnp.dot(normed[...], wq[:, c * step : (c + 1) * step], preferred_element_type=F32)
        for h in range(2):
            base = (2 * c + h) * block
            q[base : base + block, :] = rotate(qp[:, h * hd : (h + 1) * hd], qgain[...])

    factor = hd**-0.5 * math.log2(math.e)

    def fold(slot, first):
        low = slot - slot % 2
        keys = kv[0, pl.ds(low, 2)].reshape(2 * block, hd)
        values = kv[1, pl.ds(low, 2)].reshape(2 * block, hd)
        for h in range(heads):
            span = slice(h * block, (h + 1) * block)
            s = lax.dot_general(
                q[span, :], keys, (((1,), (1,)), ((), ())), preferred_element_type=F32
            )
            w = jnp.exp2(s * factor)
            d = w[:, :hd]
            for j in range(1, 2 * block // hd):
                d = d + w[:, j * hd : (j + 1) * hd]
            v = jnp.dot(w.astype(BF16), values, preferred_element_type=F32)
            if first:
                den[span, :] = d
                num[span, :] = v
            else:
                den[span, :] += d
                num[span, :] += v

    def fold_group(slot, first):
        low = slot - slot % kvx.size
        for j in range(0, kvx.size, 2):
            fold(low + j, first and j == 0)

    repeat(1, kvx.groups, kvx.forward)
    for j in range(1, kvx.size):
        kvx.wait_slot(kvx.mate(j))
    fold_group(sp, True)

    def other(i):
        for j in range(1, kvx.size):
            kvx.wait_slot(kvx.source(i, j))
        fold_group(kvx.source(i), False)

    repeat(1, kvx.groups, other)

    for h in range(heads):
        span = slice(h * block, (h + 1) * block)
        total = jnp.sum(den[span, :], axis=-1, keepdims=True)
        att[:, h * hd : (h + 1) * hd] = (num[span, :] / total).astype(BF16)

    copies[9].wait()
    chunks, chunk = part.shape[0], part.shape[3]

    def share(c, k):
        target = lax.rem(tp + k, n_tp)
        return pltpu.make_async_remote_copy(
            src_ref=part.at[c, target],
            dst_ref=got.at[c, k - 1],
            send_sem=rs_send.at[c, k - 1],
            recv_sem=rs_recv.at[c, k - 1],
            device_id={"tp": target},
            device_id_type=MESH,
        )

    order = [n_tp // 2] + [k for k in range(1, n_tp) if k != n_tp // 2]
    for c in range(chunks):
        p = jnp.dot(att[...], wo[:, c * chunk : (c + 1) * chunk], preferred_element_type=F32)
        own[c] = p.reshape(n_tp, rows, chunk)
        part[c] = p.astype(BF16).reshape(n_tp, rows, chunk)
        for k in order:
            share(c, k).start()
    for c in range(chunks):
        total = own[c, tp]
        for k in order:
            share(c, k).wait_recv()
            total = total + got[c, k - 1].astype(F32)
        out[:, c * chunk : (c + 1) * chunk] = total.astype(BF16)

    for c in range(chunks):
        for k in order:
            share(c, k).wait_send()
    tokx.finish()
    kvx.finish()


def solution(mesh):
    n_sp, n_tp = mesh.shape["sp"], mesh.shape["tp"]

    def per_device(tokens, norm_gain, wq, wk, wv, query_gain, key_gain, wo):
        rows, width = tokens.shape
        hd = query_gain.shape[0]
        block = rows * n_tp
        heads = wq.shape[1] // hd
        out_width = wo.shape[1]
        chunks = 4
        chunk = out_width // chunks
        row_np, col_np = angle_tables(block * n_sp // GRID_W, hd)
        vmem = pltpu.VMEM
        dma = pltpu.SemaphoreType.DMA
        any_spec = pl.BlockSpec(memory_space=pl.ANY)
        return pl.pallas_call(
            functools.partial(layer_kernel, n_sp, n_tp),
            out_shape=jax.ShapeDtypeStruct((rows, out_width), BF16),
            in_specs=[any_spec] * 10,
            out_specs=pl.BlockSpec(memory_space=pltpu.VMEM),
            scratch_shapes=[
                vmem((1, n_tp, rows, width), BF16),
                vmem((1, width), F32),
                vmem((1, hd), F32),
                vmem((1, hd), F32),
                vmem(wq.shape, BF16),
                vmem((width, 2 * hd), BF16),
                vmem(wo.shape, BF16),
                vmem(row_np.shape, F32),
                vmem(col_np.shape, F32),
                vmem((block, width), BF16),
                vmem((2, n_sp, block, hd), BF16),
                vmem((heads * block, hd), BF16),
                vmem((heads * block, hd), F32),
                vmem((heads * block, hd), F32),
                vmem((block, heads * hd), BF16),
                vmem((chunks, n_tp, rows, chunk), F32),
                vmem((chunks, n_tp, rows, chunk), BF16),
                vmem((chunks, n_tp - 1, rows, chunk), BF16),
                dma((10,)),
                dma((1, n_tp)),
                dma((1, n_tp)),
                dma((2, n_sp)),
                dma((2, n_sp)),
                dma((chunks, n_tp - 1)),
                dma((chunks, n_tp - 1)),
            ],
            compiler_params=pltpu.CompilerParams(
                collective_id=0, has_side_effects=True, vmem_limit_bytes=60 * 1024 * 1024
            ),
        )(
            tokens,
            norm_gain.reshape(1, width),
            wq,
            wk,
            wv,
            query_gain.reshape(1, hd),
            key_gain.reshape(1, hd),
            wo,
            jnp.asarray(row_np),
            jnp.asarray(col_np),
        )

    return jax.shard_map(
        per_device,
        mesh=mesh,
        in_specs=(
            P(("sp", "tp"), None),
            P(),
            P(None, "tp"),
            P(None, "tp"),
            P(None, "tp"),
            P(),
            P(),
            P("tp", None),
        ),
        out_specs=P(("sp", "tp"), None),
        check_vma=False,
    )
```

```python
import functools
import math

import jax
import jax.numpy as jnp
import numpy as np
from jax import lax
from jax.experimental import pallas as pl
from jax.experimental.pallas import tpu as pltpu

from jax.sharding import PartitionSpec as P

GRID_W = 64
EPS = 1e-06
ROTARY_BASE = 10000.0
MESH = pl.DeviceIdType.MESH
F32 = jnp.float32
BF16 = jnp.bfloat16
UNROLL = 8


def angle_tables(grid_rows, head_dim):
    half = head_dim // 2
    freq = np.float32(ROTARY_BASE) ** (-np.arange(0, half, 2, dtype=np.float32) / np.float32(half))
    freq = np.repeat(freq.astype(np.float32), 2)
    sign = np.tile(np.array([-1.0, 1.0], np.float32), half // 2)
    zero = lambda n: np.zeros((n, half), np.float32)
    row = np.arange(grid_rows, dtype=np.float32)[:, None] * freq[None, :]
    col = np.arange(GRID_W, dtype=np.float32)[:, None] * freq[None, :]
    rows = np.stack(
        [
            np.concatenate([np.cos(row), zero(grid_rows)], 1),
            np.concatenate([np.sin(row) * sign, zero(grid_rows)], 1),
        ]
    )
    cols = np.stack(
        [
            np.concatenate([zero(GRID_W), np.cos(col)], 1),
            np.concatenate([zero(GRID_W), np.sin(col) * sign], 1),
        ]
    )
    return rows.astype(np.float32), cols.astype(np.float32)


def repeat(start, stop, body):
    if stop - start <= UNROLL:
        for i in range(start, stop):
            body(i)
    else:
        lax.fori_loop(start, stop, lambda i, c: (body(i), c)[1], 0)


class GroupExchange:
    def __init__(self, axis, n, size, buf, send, recv):
        self.axis, self.size, self.buf, self.send, self.recv = axis, size, buf, send, recv
        self.groups = n // size
        self.me = lax.axis_index(axis)
        self.group, self.place = self.me // size, self.me % size
        self.parts = buf.shape[0]

    def mate(self, j):
        return self.group * self.size + lax.rem(self.place + j, self.size)

    def peer(self, i):
        return lax.rem(self.group + i, self.groups) * self.size + self.place

    def source(self, i, j=0):
        group = lax.rem(self.group + self.groups - i, self.groups)
        return group * self.size + lax.rem(self.place + j, self.size)

    def copy(self, part, slot, sem, target):
        return pltpu.make_async_remote_copy(
            src_ref=self.buf.at[part, slot],
            dst_ref=self.buf.at[part, slot],
            send_sem=self.send.at[part, sem],
            recv_sem=self.recv.at[part, slot],
            device_id={self.axis: target},
            device_id_type=MESH,
        )

    def greet(self, barrier):
        def one(target):
            pl.semaphore_signal(barrier, inc=1, device_id={self.axis: target}, device_id_type=MESH)

        repeat(1, self.groups, lambda i: one(self.peer(i)))
        for j in range(1, self.size):
            one(self.mate(j))
        return self.groups + self.size - 2

    def start(self):
        def one(i):
            for part in range(self.parts):
                self.copy(part, self.me, self.size - 2 + i, self.peer(i)).start()

        repeat(1, self.groups, one)
        for j in range(1, self.size):
            for part in range(self.parts):
                self.copy(part, self.me, j - 1, self.mate(j)).start()

    def forward(self, i):
        slot = self.source(i)
        first = self.groups + self.size - 2 + (i - 1) * (self.size - 1)
        for part in range(self.parts):
            self.copy(part, slot, 0, self.peer(i)).wait_recv()
            for j in range(1, self.size):
                self.copy(part, slot, first + j - 1, self.mate(j)).start()

    def wait_slot(self, slot):
        for part in range(self.parts):
            self.copy(part, slot, 0, self.mate(1)).wait_recv()

    def finish(self):
        def one(i):
            for part in range(self.parts):
                self.copy(part, self.me, i, self.mate(1)).wait_send()

        repeat(0, self.groups * self.size - 1, one)


def layer_kernel(
    n_sp,
    n_tp,
    tokens,
    norm_gain,
    wq_hbm,
    wk_hbm,
    wv_hbm,
    query_gain,
    key_gain,
    wo_hbm,
    row_hbm,
    col_hbm,
    out,
    tok,
    gain,
    qgain,
    kgain,
    wq,
    wkv,
    wo,
    rowtab,
    coltab,
    normed,
    kv,
    q,
    num,
    den,
    att,
    own,
    part,
    got,
    lsem,
    tok_send,
    tok_recv,
    kv_send,
    kv_recv,
    rs_send,
    rs_recv,
):
    tp = lax.axis_index("tp")
    sp = lax.axis_index("sp")
    rows, width = tok.shape[2], tok.shape[3]
    block = n_tp * rows
    hd = q.shape[1]
    heads = wq.shape[1] // hd
    tokx = GroupExchange("tp", n_tp, n_tp, tok, tok_send, tok_recv)
    kvx = GroupExchange("sp", n_sp, 4, kv, kv_send, kv_recv)

    local = [
        (tokens, tok.at[0, tp]),
        (norm_gain, gain),
        (wk_hbm, wkv.at[:, pl.ds(0, hd)]),
        (wv_hbm, wkv.at[:, pl.ds(hd, hd)]),
        (key_gain, kgain),
        (query_gain, qgain),
        (row_hbm, rowtab),
        (col_hbm, coltab),
        (wq_hbm, wq),
        (wo_hbm, wo),
    ]
    copies = [pltpu.make_async_copy(a, b, lsem.at[i]) for i, (a, b) in enumerate(local)]
    barrier = pltpu.get_barrier_semaphore()
    copies[0].start()
    count = kvx.greet(barrier) + n_tp - 1
    for k in range(1, n_tp):
        target = lax.rem(tp + k, n_tp)
        pl.semaphore_signal(barrier, inc=1, device_id={"tp": target}, device_id_type=MESH)
    for c in copies[1:]:
        c.start()
    copies[0].wait()
    pl.semaphore_wait(barrier, count)

    tokx.start()

    for c in copies[1:8]:
        c.wait()
    grid_rows = block // GRID_W
    cosine, sine = [], []
    for g in range(grid_rows):
        r = sp * grid_rows + g
        cosine.append(coltab[0] + rowtab[0, pl.ds(r, 1), :])
        sine.append(coltab[1] + rowtab[1, pl.ds(r, 1), :])
    cosine = jnp.concatenate(cosine, 0)
    sine = jnp.concatenate(sine, 0)
    even = lax.broadcasted_iota(jnp.int32, (block, hd), 1) % 2 == 0

    def rotate(projected, head_gain):
        x = projected.astype(BF16).astype(F32)
        x = x * lax.rsqrt(jnp.mean(x * x, axis=-1, keepdims=True) + EPS) * head_gain
        swapped = jnp.where(even, pltpu.roll(x, hd - 1, 1), pltpu.roll(x, 1, 1))
        return (x * cosine + swapped * sine).astype(BF16)

    def norm(slot):
        x = tok[0, slot].astype(F32)
        x = x * lax.rsqrt(jnp.mean(x * x, axis=-1, keepdims=True) + EPS) * gain[...]
        start = pl.multiple_of(slot * rows, rows)
        normed[pl.ds(start, rows), :] = x.astype(BF16)

    norm(tp)
    for i in range(1, tokx.groups):
        tokx.forward(i)
        norm(tokx.source(i))
    for j in range(1, tokx.size):
        tokx.wait_slot(tokx.mate(j))
        norm(tokx.mate(j))
    for i in range(1, tokx.groups):
        for j in range(1, tokx.size):
            tokx.wait_slot(tokx.source(i, j))
            norm(tokx.source(i, j))

    kvp = jnp.dot(normed[...], wkv[...], preferred_element_type=F32)
    kv[1, sp] = kvp[:, hd:].astype(BF16)
    kv[0, sp] = rotate(kvp[:, :hd], kgain[...])
    kvx.start()

    copies[8].wait()
    step = 2 * hd
    for c in range(wq.shape[1] // step):
        qp = jnp.dot(normed[...], wq[:, c * step : (c + 1) * step], preferred_element_type=F32)
        for h in range(2):
            base = (2 * c + h) * block
            q[base : base + block, :] = rotate(qp[:, h * hd : (h + 1) * hd], qgain[...])

    factor = hd**-0.5 * math.log2(math.e)

    def fold(slot, first):
        low = slot - slot % 2
        keys = kv[0, pl.ds(low, 2)].reshape(2 * block, hd)
        values = kv[1, pl.ds(low, 2)].reshape(2 * block, hd)
        for h in range(heads):
            span = slice(h * block, (h + 1) * block)
            s = lax.dot_general(
                q[span, :], keys, (((1,), (1,)), ((), ())), preferred_element_type=F32
            )
            w = jnp.exp2(s * factor)
            d = w[:, :hd]
            for j in range(1, 2 * block // hd):
                d = d + w[:, j * hd : (j + 1) * hd]
            v = jnp.dot(w.astype(BF16), values, preferred_element_type=F32)
            if first:
                den[span, :] = d
                num[span, :] = v
            else:
                den[span, :] += d
                num[span, :] += v

    def fold_group(slot, first):
        low = slot - slot % kvx.size
        for j in range(0, kvx.size, 2):
            fold(low + j, first and j == 0)

    repeat(1, kvx.groups, kvx.forward)
    for j in range(1, kvx.size):
        kvx.wait_slot(kvx.mate(j))
    fold_group(sp, True)

    def other(i):
        for j in range(1, kvx.size):
            kvx.wait_slot(kvx.source(i, j))
        fold_group(kvx.source(i), False)

    repeat(1, kvx.groups, other)

    for h in range(heads):
        span = slice(h * block, (h + 1) * block)
        total = jnp.sum(den[span, :], axis=-1, keepdims=True)
        att[:, h * hd : (h + 1) * hd] = (num[span, :] / total).astype(BF16)

    copies[9].wait()
    chunks, chunk = part.shape[0], part.shape[3]

    def share(c, k):
        target = lax.rem(tp + k, n_tp)
        return pltpu.make_async_remote_copy(
            src_ref=part.at[c, target],
            dst_ref=got.at[c, k - 1],
            send_sem=rs_send.at[c, k - 1],
            recv_sem=rs_recv.at[c, k - 1],
            device_id={"tp": target},
            device_id_type=MESH,
        )

    order = [n_tp // 2] + [k for k in range(1, n_tp) if k != n_tp // 2]
    for c in range(chunks):
        p = jnp.dot(att[...], wo[:, c * chunk : (c + 1) * chunk], preferred_element_type=F32)
        own[c] = p.reshape(n_tp, rows, chunk)
        part[c] = p.astype(BF16).reshape(n_tp, rows, chunk)
        for k in order:
            share(c, k).start()
    for c in range(chunks):
        total = own[c, tp]
        for k in order:
            share(c, k).wait_recv()
            total = total + got[c, k - 1].astype(F32)
        out[:, c * chunk : (c + 1) * chunk] = total.astype(BF16)

    for c in range(chunks):
        for k in order:
            share(c, k).wait_send()
    tokx.finish()
    kvx.finish()


def solution(mesh):
    n_sp, n_tp = mesh.shape["sp"], mesh.shape["tp"]

    def per_device(tokens, norm_gain, wq, wk, wv, query_gain, key_gain, wo):
        rows, width = tokens.shape
        hd = query_gain.shape[0]
        block = rows * n_tp
        heads = wq.shape[1] // hd
        out_width = wo.shape[1]
        chunks = 2
        chunk = out_width // chunks
        row_np, col_np = angle_tables(block * n_sp // GRID_W, hd)
        vmem = pltpu.VMEM
        dma = pltpu.SemaphoreType.DMA
        any_spec = pl.BlockSpec(memory_space=pl.ANY)
        return pl.pallas_call(
            functools.partial(layer_kernel, n_sp, n_tp),
            out_shape=jax.ShapeDtypeStruct((rows, out_width), BF16),
            in_specs=[any_spec] * 10,
            out_specs=pl.BlockSpec(memory_space=pltpu.VMEM),
            scratch_shapes=[
                vmem((1, n_tp, rows, width), BF16),
                vmem((1, width), F32),
                vmem((1, hd), F32),
                vmem((1, hd), F32),
                vmem(wq.shape, BF16),
                vmem((width, 2 * hd), BF16),
                vmem(wo.shape, BF16),
                vmem(row_np.shape, F32),
                vmem(col_np.shape, F32),
                vmem((block, width), BF16),
                vmem((2, n_sp, block, hd), BF16),
                vmem((heads * block, hd), BF16),
                vmem((heads * block, hd), F32),
                vmem((heads * block, hd), F32),
                vmem((block, heads * hd), BF16),
                vmem((chunks, n_tp, rows, chunk), F32),
                vmem((chunks, n_tp, rows, chunk), BF16),
                vmem((chunks, n_tp - 1, rows, chunk), BF16),
                dma((10,)),
                dma((1, n_tp)),
                dma((1, n_tp)),
                dma((2, n_sp)),
                dma((2, n_sp)),
                dma((chunks, n_tp - 1)),
                dma((chunks, n_tp - 1)),
            ],
            compiler_params=pltpu.CompilerParams(
                collective_id=0, has_side_effects=True, vmem_limit_bytes=60 * 1024 * 1024
            ),
        )(
            tokens,
            norm_gain.reshape(1, width),
            wq,
            wk,
            wv,
            query_gain.reshape(1, hd),
            key_gain.reshape(1, hd),
            wo,
            jnp.asarray(row_np),
            jnp.asarray(col_np),
        )

    return jax.shard_map(
        per_device,
        mesh=mesh,
        in_specs=(
            P(("sp", "tp"), None),
            P(),
            P(None, "tp"),
            P(None, "tp"),
            P(None, "tp"),
            P(),
            P(),
            P("tp", None),
        ),
        out_specs=P(("sp", "tp"), None),
        check_vma=False,
    )
```
